32 devices in a mesh: ep: 8 (over z, y), tp: 4 (over x, core).
Axes of the slice: x: 2, y: 2, z: 4, core: 2. Of those that a mesh axis runs over, the one named last changes fastest.
Arguments:
- query_rows: bfloat16 [4096, 1024], P('ep', 'tp'), may hold values from -10 to 10
- key_rows: bfloat16 [4096, 1024], P('ep', 'tp'), may hold values from -10 to 10
- value_rows: bfloat16 [4096, 1024], P('ep', 'tp'), may hold values from -6 to 6
- key_bias: float32 [4096, 16], P(None, 'tp'), may hold values from -30 to 0
- out_weight: bfloat16 [1024, 2048], P('tp'), may hold values from -0.5625 to 0.5625
- moe_input: bfloat16 [4096, 2048], P(('ep', 'tp')), may hold values from -6 to 6
- moe_gain: float32 [2048], replicated, may hold values from 0.1 to 1.9
- expert_pick: int32 [4096, 2], P(('ep', 'tp')), may hold values from 0 to 7, as said below
- route_weight: float32 [4096, 2], P(('ep', 'tp')), may hold values from 0.1 to 1
- w_gate: bfloat16 [8, 2048, 1024], P('ep', None, 'tp'), may hold values from -0.125 to 0.125
- w_up: bfloat16 [8, 2048, 1024], P('ep', None, 'tp'), may hold values from -0.125 to 0.125
- w_down: bfloat16 [8, 1024, 2048], P('ep', 'tp'), may hold values from -0.1875 to 0.1875
Outputs:
- mixer_out: bfloat16 [4096, 2048], P(('ep', 'tp'))
- routed_out: bfloat16 [4096, 2048], P(('ep', 'tp'))
The draws below stay inside these ranges and needn't reach their ends.
Inputs may be any that keep to these rules, and one draw needn't show every extreme that they name: `expert_pick`: each row names two different experts of one group, expert e belonging to group e // 2; the rows of one device name no expert more than 64 times, and in every draw each expert of some group is named exactly 64 times by the rows of every device.
All inputs are finite; a program needn't handle non-finite values.
Results may differ from the reference program's by a relative error of at most 0.013.
Values may be sent and summed in bfloat16 or wider, within the bound.
No kernel may reach another device: no remote copies, remote signals or barrier semaphores. Data moves between devices by JAX's collectives and lax.ppermute only.
A program may use at most 128 MiB of HBM per device.

```python
import math
import jax
import jax.numpy as jnp
from jax import lax

D = 2048
ATTENTION_HEADS = 16
HEAD_DIM = 64
FF = 1024
GROUPS = 4
TOPK = 2
SEQ_DEV = 512
TOK2_DEV = 128
EXPERTS = 8
FIRST_TOKENS1 = 4096
SEQ_BLOCKS = 8
TOKENS2 = 4096
CAP = 64
N_TP = 4


def draw_key_bias(key, part):
    flow_lanes = jax.random.split(jax.random.fold_in(key, 101), 5)
    fast_heads = jax.random.uniform(flow_lanes[0], (ATTENTION_HEADS,)) < 0.5
    jitter = jnp.clip(0.5 * jax.random.normal(flow_lanes[2], (FIRST_TOKENS1, ATTENTION_HEADS)), -1.0, 1.0)
    base_level = jnp.where(fast_heads, -jnp.log(4000.0), -jnp.log(130.0 * FIRST_TOKENS1))
    block_count = FIRST_TOKENS1 // SEQ_DEV
    shifts = jax.random.uniform(flow_lanes[1], (block_count, 1, ATTENTION_HEADS), minval=-0.75, maxval=0.75)
    shifts = jnp.broadcast_to(shifts, (block_count, SEQ_DEV, ATTENTION_HEADS)).reshape(FIRST_TOKENS1, ATTENTION_HEADS)
    bias_terms = base_level[None, :] + shifts + jitter
    slot_places = jax.random.randint(flow_lanes[3], (3, ATTENTION_HEADS), 0, FIRST_TOKENS1, dtype=jnp.int32)
    token_positions = jnp.arange(FIRST_TOKENS1, dtype=jnp.int32)[:, None]
    spike_mask = (token_positions == slot_places[0][None, :]) | (token_positions == slot_places[1][None, :]) | (token_positions == slot_places[2][None, :])
    spike_level = jax.random.uniform(flow_lanes[4], (FIRST_TOKENS1, ATTENTION_HEADS), minval=-2.0, maxval=-1.0)
    return jnp.where(spike_mask, spike_level, bias_terms).astype(jnp.float32)


def draw_expert_pick(key, part):
    base_key = jax.random.fold_in(key, 202)
    group_size = EXPERTS // GROUPS
    half_rows = TOK2_DEV // 2
    block_count = TOKENS2 // TOK2_DEV
    favored = jax.random.randint(jax.random.fold_in(base_key, 1), (), 0, GROUPS, dtype=jnp.int32)

    def one_block(block_key):
        flow_lanes = jax.random.split(block_key, 4)
        cut_points = jnp.sort(jax.random.randint(flow_lanes[0], (GROUPS - 2,), 0, half_rows + 1, dtype=jnp.int32))
        bounds = jnp.concatenate([jnp.zeros((1,), jnp.int32), cut_points, jnp.full((1,), half_rows, jnp.int32)])
        others = (favored + 1 + jnp.arange(GROUPS - 1, dtype=jnp.int32)) % GROUPS
        counts = jnp.zeros((GROUPS,), jnp.int32).at[favored].set(half_rows).at[others].set(bounds[1:] - bounds[:-1])
        group_ends = jnp.cumsum(counts)
        starts = group_ends - counts
        token_positions = jnp.arange(TOK2_DEV, dtype=jnp.int32)
        group_id = jnp.sum((token_positions[:, None] >= group_ends[None, :]).astype(jnp.int32), axis=1)
        group_rank = token_positions - starts[group_id]
        rotation = jax.random.randint(flow_lanes[1], (GROUPS,), 0, group_size, dtype=jnp.int32)
        offset = jax.random.randint(flow_lanes[2], (GROUPS,), 1, group_size, dtype=jnp.int32)
        first_pick = (group_rank + rotation[group_id]) % group_size
        second = (group_rank + rotation[group_id] + offset[group_id]) % group_size
        picked = jnp.stack([group_id * group_size + first_pick, group_id * group_size + second], axis=1)
        return picked[jax.random.permutation(flow_lanes[3], TOK2_DEV)]
    blocks = jax.vmap(one_block)(jax.random.split(base_key, block_count))
    return blocks.reshape(TOKENS2, TOPK).astype(jnp.int32)


def shard_levels(own_key, shape, cuts, least, top_value):
    gain = 1.0
    for dim, parts in cuts:
        heights = jax.random.uniform(jax.random.fold_in(jax.random.fold_in(own_key, 6), dim), (parts,), jnp.float32, least / len(cuts), top_value / len(cuts))
        gain = gain * jnp.repeat(jnp.exp(heights), shape[dim] // parts).reshape((-1,) + (1,) * (len(shape) - 1 - dim))
    return gain


def bell_draw(key, extent, spread, bound, shards=(), kind=jnp.bfloat16):
    drawn = jax.random.normal(key, extent, jnp.float32) * spread
    if len(shards) > 0:
        drawn = shard_levels(key, extent, shards, -0.22, 0.18) * drawn
    return jnp.clip(drawn, min=-bound, max=bound).astype(kind)


def setup_inputs(seed: int = 0) -> dict:
    keys = jax.random.split(jax.random.key(seed), 13)
    return {
        "query_rows": bell_draw(keys[0], (FIRST_TOKENS1, ATTENTION_HEADS * HEAD_DIM), 1.7, 10.0, ((0, 8), (1, 4))),
        "key_rows": bell_draw(keys[1], (FIRST_TOKENS1, ATTENTION_HEADS * HEAD_DIM), 1.7, 10.0, ((0, 8), (1, 4))),
        "value_rows": bell_draw(keys[2], (FIRST_TOKENS1, ATTENTION_HEADS * HEAD_DIM), 1.0, 6.0, ((0, 8), (1, 4))),
        "key_bias": draw_key_bias(jax.random.fold_in(keys[12], 71), 0),
        "out_weight": bell_draw(keys[4], (ATTENTION_HEADS * HEAD_DIM, D), (3.0 * (ATTENTION_HEADS * HEAD_DIM) ** -0.5), 0.5625, ((0, 4),)),
        "moe_input": bell_draw(keys[5], (TOKENS2, D), 1.0, 6.0, ((0, 32),)),
        "moe_gain": jnp.clip(1.0 + 0.18 * jax.random.normal(keys[6], (D,), jnp.float32), 0.1, 1.9),
        "expert_pick": draw_expert_pick(jax.random.fold_in(keys[12], 71), 0),
        "route_weight": jnp.clip(jnp.exp(math.log(1.0) - 2.3025851 * jax.random.uniform(keys[8], (TOKENS2, TOPK), jnp.float32) ** shard_levels(keys[8], (TOKENS2, TOPK), ((0, 32),), -0.2, 0.2)), 0.1, 1.0),
        "w_gate": bell_draw(keys[9], (EXPERTS, D, FF), D ** -0.5, 0.125, ((0, 8), (2, 4))),
        "w_up": bell_draw(keys[10], (EXPERTS, D, FF), D ** -0.5, 0.125, ((0, 8), (2, 4))),
        "w_down": bell_draw(keys[11], (EXPERTS, FF, D), FF ** -0.5, 0.1875, ((0, 8), (1, 4))),
    }


def block_values(query_heads, query_first, key_heads, value_heads, bias_heads, key_first, running):
    scores = jnp.einsum('hqd,hkd->hqk', query_heads.astype(jnp.float32), key_heads.astype(jnp.float32))
    scores = scores * HEAD_DIM ** (-0.5) + bias_heads[:, None, :]
    query_pos = query_first + jnp.arange(query_heads.shape[1], dtype=jnp.int32)
    key_pos = key_first + jnp.arange(key_heads.shape[1], dtype=jnp.int32)
    causal = (key_pos[None, :] < query_pos[:, None])[None]
    failure = jnp.where(causal, jax.nn.log_sigmoid(-scores), 0.0)
    remainder = lax.cumsum(failure, axis=2, reverse=True) - failure + running[:, :, None]
    stick_weight = jnp.where(causal, jnp.exp(jax.nn.log_sigmoid(scores) + remainder), 0.0).astype(jnp.bfloat16)
    portion = jnp.einsum('hqk,hkd->hqd', stick_weight.astype(jnp.float32), value_heads.astype(jnp.float32))
    return (portion, running + lax.optimization_barrier(jnp.sum(failure, axis=2)))

def mixer(query_rows, key_rows, value_rows, key_bias, out_weight):
    block_count = FIRST_TOKENS1 // SEQ_DEV

    def split_heads(rows):
        return jnp.transpose(rows.reshape(block_count, SEQ_DEV, ATTENTION_HEADS, HEAD_DIM), (0, 2, 1, 3))
    query_heads = split_heads(query_rows)
    key_heads = split_heads(key_rows)
    value_heads = split_heads(value_rows)
    bias_heads = jnp.transpose(key_bias.reshape(block_count, SEQ_DEV, ATTENTION_HEADS), (0, 2, 1))

    def one_block(block_index):

        def visit(step_index, carried):
            source = block_index - step_index
            portion, running = block_values(query_heads[block_index], block_index * SEQ_DEV, key_heads[source], value_heads[source], bias_heads[source], source * SEQ_DEV, carried[1])
            return (carried[0] + portion, running)
        start_state = (jnp.zeros((ATTENTION_HEADS, SEQ_DEV, HEAD_DIM), jnp.float32), jnp.zeros((ATTENTION_HEADS, SEQ_DEV), jnp.float32))
        steps_here = block_index % SEQ_BLOCKS + 1
        return lax.fori_loop(0, steps_here, visit, start_state)[0].astype(jnp.bfloat16)
    attended = lax.map(one_block, jnp.arange(block_count, dtype=jnp.int32))
    attended = jnp.transpose(attended, (0, 2, 1, 3)).reshape(FIRST_TOKENS1, ATTENTION_HEADS * HEAD_DIM)
    group_width = ATTENTION_HEADS * HEAD_DIM // N_TP
    summed = jnp.zeros((FIRST_TOKENS1, D), jnp.float32)
    for group in range(N_TP):
        columns = attended[:, group * group_width:(group + 1) * group_width]
        weights = out_weight[group * group_width:(group + 1) * group_width]
        rounded = jnp.dot(columns, weights, preferred_element_type=jnp.float32).astype(jnp.bfloat16)
        summed = summed + lax.optimization_barrier(rounded).astype(jnp.float32)
    return summed.astype(jnp.bfloat16)

def experts(moe_input, moe_gain, expert_pick, route_weight, w_gate, w_up, w_down):
    widened = moe_input.astype(jnp.float32)
    normed = (widened * lax.rsqrt(lax.optimization_barrier(jnp.mean(widened * widened, axis=1, keepdims=True)) + 1e-06) * moe_gain).astype(jnp.bfloat16)
    block_count = TOKENS2 // TOK2_DEV
    picks = expert_pick.reshape(block_count, TOK2_DEV * TOPK)
    matches = (picks[:, :, None] == jnp.arange(EXPERTS, dtype=jnp.int32)[None, None, :]).astype(jnp.int32)
    ranks = lax.optimization_barrier(jnp.sum((jnp.cumsum(matches, axis=1) - matches) * matches, axis=2))
    block_ids = jnp.arange(block_count, dtype=jnp.int32)[:, None]
    slots = picks * (block_count * CAP) + block_ids * CAP + ranks
    owners = block_ids * TOK2_DEV + jnp.arange(TOK2_DEV * TOPK, dtype=jnp.int32)[None, :] // TOPK
    table = jnp.full((EXPERTS * block_count * CAP,), TOKENS2, jnp.int32)
    table = table.at[slots.reshape(-1)].set(owners.reshape(-1)).reshape(EXPERTS, block_count * CAP)
    padded = jnp.concatenate([normed, jnp.zeros((1, D), jnp.bfloat16)], axis=0)

    def serve(expert):
        rows = padded[table[expert]]
        gate_in = jnp.dot(rows, w_gate[expert], preferred_element_type=jnp.float32)
        up_in = jnp.dot(rows, w_up[expert], preferred_element_type=jnp.float32)
        hidden = (jax.nn.silu(gate_in) * up_in).astype(jnp.bfloat16)
        return jnp.dot(hidden, w_down[expert], preferred_element_type=jnp.float32).astype(jnp.bfloat16)
    served = lax.map(serve, jnp.arange(EXPERTS, dtype=jnp.int32))
    chosen = served.reshape(EXPERTS * block_count * CAP, D)[slots.reshape(-1)]
    chosen = chosen.reshape(TOKENS2, TOPK, D).astype(jnp.float32)
    return lax.optimization_barrier(jnp.sum(chosen * route_weight[:, :, None], axis=1)).astype(jnp.bfloat16)

def reference(query_rows, key_rows, value_rows, key_bias, out_weight, moe_input, moe_gain, expert_pick, route_weight, w_gate, w_up, w_down):
    return (mixer(query_rows, key_rows, value_rows, key_bias, out_weight), experts(moe_input, moe_gain, expert_pick, route_weight, w_gate, w_up, w_down))
```

```python
import functools
import math

import jax
import jax.numpy as jnp
from jax import lax
from jax.experimental import pallas as pl
from jax.experimental.pallas import tpu as pltpu
from jax.sharding import PartitionSpec as P

HEAD_DIM = 64
GROUPS = 4
TOPK = 2
LANES = 128
KEY_TILE = 256
LOG2E = math.log2(math.e)
MIB = 1 << 20

norm_eps = 1e-06
bf16 = jnp.bfloat16
f32 = jnp.float32

VMEM = pl.BlockSpec(memory_space=pltpu.VMEM)
SMEM = pl.BlockSpec(memory_space=pltpu.SMEM)


def call(body, name, outs, ins, limit, flops=0, moved=0):
    return pl.pallas_call(
        body,
        name=name,
        out_shape=outs,
        in_specs=ins,
        out_specs=jax.tree.map(lambda _: VMEM, outs),
        compiler_params=pltpu.CompilerParams(vmem_limit_bytes=limit * MIB),
        cost_estimate=pl.CostEstimate(flops=flops, bytes_accessed=moved, transcendentals=0),
    )


def mm(a, b):
    return jnp.dot(a, b, preferred_element_type=f32)


def pack_body(q_ref, k_ref, v_ref, out_ref, *, heads, sharers, parts):
    rows = q_ref.shape[0]
    part_rows = rows // parts
    sub = part_rows // sharers
    half = rows // sharers // 2
    for h in range(heads):
        cols = pl.ds(h * HEAD_DIM, HEAD_DIM)
        pair = jnp.concatenate([k_ref[:, cols], v_ref[:, cols]], axis=1)
        for s in range(sharers):
            out_ref[h * sharers + s, :rows] = pair
            mine = jnp.concatenate(
                [q_ref[pl.ds(t * part_rows + s * sub, sub), cols] for t in range(parts)], axis=0
            )
            out_ref[h * sharers + s, rows:] = jnp.concatenate([mine[:half], mine[half:]], axis=1)


def attend_body(where_ref, got_ref, bias_ref, out_ref, *, rows, sub, parts):
    blocks = got_ref.shape[0]
    mine = sub * parts
    half = mine // 2
    share = where_ref[0]
    scale = HEAD_DIM**-0.5 * LOG2E
    tiles = rows // KEY_TILE
    part_rows = rows // parts
    low = lax.broadcasted_iota(jnp.int32, (half, LANES), 1) < HEAD_DIM
    later = (
        lax.broadcasted_iota(jnp.int32, (KEY_TILE, KEY_TILE), 0)
        > lax.broadcasted_iota(jnp.int32, (KEY_TILE, KEY_TILE), 1)
    )
    after = jnp.where(later, 1.0, 0.0).astype(bf16)
    row = lax.broadcasted_iota(jnp.int32, (mine, KEY_TILE), 0)
    spot = row + share * sub
    for t in range(1, parts):
        spot = spot + jnp.where(row >= t * sub, part_rows - sub, 0)
    lane = lax.broadcasted_iota(jnp.int32, (mine, KEY_TILE), 1)

    def tile(query, source, c, masked):
        pair = got_ref[source, pl.ds(c * KEY_TILE, KEY_TILE)]
        bias = bias_ref[pl.ds(source * tiles + c, 1)]
        raw = lax.dot_general(query, pair, (((1,), (1,)), ((), ())), preferred_element_type=f32)
        score = raw * scale + bias
        soft = jnp.maximum(score, 0.0) + jnp.log2(1.0 + jnp.exp2(-jnp.abs(score)))
        if masked:
            causal = lane + c * KEY_TILE < spot
            soft = jnp.where(causal, soft, 0.0)
        rounded = soft.astype(bf16)
        rest = mm(rounded, after)
        weight = jnp.exp2(score - soft - rest)
        if masked:
            weight = jnp.where(causal, weight, 0.0)
        total = rest[:, :1] + rounded[:, :1].astype(f32)
        return mm(weight.astype(bf16), pair), total

    def visit(query, source, state, masked):
        found = [tile(query, source, c, masked) for c in reversed(range(tiles))]
        acc, carry = state
        for portion, total in found:
            acc = acc + portion * jnp.exp2(-carry)
            carry = carry + total
        return acc, carry

    def one_block(b, _):
        packed = got_ref[b, pl.ds(rows, half)].astype(f32)
        query = jnp.concatenate(
            [
                jnp.where(low, packed, 0.0),
                jnp.where(low, pltpu.roll(packed, HEAD_DIM, 1), 0.0),
            ],
            axis=0,
        ).astype(bf16)
        state = (jnp.zeros((mine, LANES), f32), jnp.zeros((mine, 1), f32))
        state = visit(query, b, state, True)
        acc, _ = lax.fori_loop(
            0, b, lambda i, st: visit(query, b - 1 - i, st, False), state
        )
        turned = pltpu.roll(acc, HEAD_DIM, 1)
        few = sub // 2
        keep = lax.broadcasted_iota(jnp.int32, (few, LANES), 1) < HEAD_DIM
        for t in range(parts):
            first = turned[t * sub : t * sub + few]
            second = acc[t * sub + few : (t + 1) * sub]
            out_ref[b, t] = jnp.where(keep, first, second).astype(bf16)
        return 0

    lax.fori_loop(0, blocks, one_block, 0)


def project_body(where_ref, got_ref, w0, w1, w2, w3, out_ref, *, heads, sharers, parts):
    here = where_ref[1]
    few = got_ref.shape[1]
    low = lax.broadcasted_iota(jnp.int32, (few, LANES), 1) < HEAD_DIM
    total = None
    for m, w_ref in enumerate((w0, w1, w2, w3)):
        tp = here ^ m
        strips = []
        for s in range(sharers):
            firsts, seconds = [], []
            for h in range(0, heads, 2):
                a = got_ref[(h * sharers + s) * parts + tp].astype(f32)
                b = got_ref[((h + 1) * sharers + s) * parts + tp].astype(f32)
                firsts.append(jnp.where(low, a, pltpu.roll(b, HEAD_DIM, 1)))
                seconds.append(jnp.where(low, pltpu.roll(a, HEAD_DIM, 1), b))
            strips.append(jnp.concatenate(firsts, axis=1))
            strips.append(jnp.concatenate(seconds, axis=1))
        left = jnp.concatenate(strips, axis=0).astype(bf16)
        part = mm(left, w_ref[...])
        total = part if total is None else total + part
    out_ref[...] = total.astype(bf16)


def spread(piece, size):
    cross = [(i, i ^ 2) for i in range(size)]
    beside = [(i, i ^ 1) for i in range(size)]
    far = lax.ppermute(piece, "tp", cross)
    near = lax.ppermute(piece, "tp", beside)
    return (piece, near, far, lax.ppermute(far, "tp", beside))


def mixer(query_rows, key_rows, value_rows, key_bias, out_pieces):
    rows = query_rows.shape[0]
    heads = query_rows.shape[1] // HEAD_DIM
    ep_count = lax.axis_size("ep")
    parts = lax.axis_size("tp")
    ep_index = lax.axis_index("ep")
    tp_index = lax.axis_index("tp")
    sharers = ep_count // heads
    sub = rows // parts // sharers
    mine = sub * parts
    tall = rows + mine // 2
    outgoing = call(
        functools.partial(pack_body, heads=heads, sharers=sharers, parts=parts),
        "pack",
        jax.ShapeDtypeStruct((ep_count, tall, LANES), bf16),
        [VMEM] * 3,
        32,
    )(query_rows, key_rows, value_rows)
    got = lax.all_to_all(outgoing, "ep", split_axis=0, concat_axis=0, tiled=True)
    head = ep_index // sharers
    bias = lax.dynamic_index_in_dim(key_bias, head, 1, keepdims=False) * LOG2E
    bias = bias.reshape(-1, KEY_TILE)
    where = jnp.stack([ep_index % sharers, tp_index]).astype(jnp.int32)
    attended = call(
        functools.partial(attend_body, rows=rows, sub=sub, parts=parts),
        "attend",
        jax.ShapeDtypeStruct((ep_count, parts, sub // 2, LANES), bf16),
        [SMEM, VMEM, VMEM],
        48,
        flops=3 * ep_count * ep_count * mine * rows * LANES,
    )(where, got, bias)
    attended = attended.reshape(ep_count * parts, sub // 2, LANES)
    back = lax.all_to_all(attended, ("ep", "tp"), split_axis=0, concat_axis=0, tiled=True)
    return call(
        functools.partial(project_body, heads=heads, sharers=sharers, parts=parts),
        "project",
        jax.ShapeDtypeStruct((rows // parts, out_pieces[0].shape[1]), bf16),
        [SMEM] + [VMEM] * 5,
        48,
        flops=2 * rows * heads * HEAD_DIM * out_pieces[0].shape[1],
    )(where, back, *out_pieces)


def route_body(zy_ref, x_ref, gain_ref, pick_t_ref, pick_ref, weight_ref, *outs, cap):
    out_refs, turn_ref = outs[:-1], outs[-1]
    tokens, width = x_ref.shape
    wide = x_ref[...].astype(f32)
    normed = (
        wide
        * lax.rsqrt(jnp.mean(wide * wide, axis=1, keepdims=True) + norm_eps)
        * gain_ref[...]
    ).astype(bf16)
    z = zy_ref[0]
    pick = pick_t_ref[0:1, :]
    lanes = GROUPS * 2
    group = lax.broadcasted_iota(jnp.int32, (lanes, tokens), 0)
    inside = (pick >= group * TOPK) & (pick < (group + 1) * TOPK)
    match = jnp.where(inside, 1.0, 0.0)
    before = (
        lax.broadcasted_iota(jnp.int32, (tokens, tokens), 0)
        < lax.broadcasted_iota(jnp.int32, (tokens, tokens), 1)
    )
    rank = mm(match.astype(bf16), jnp.where(before, 1.0, 0.0).astype(bf16))
    first = ((group ^ z) * cap).astype(f32)
    slot = jnp.sum(match * (rank + first), axis=0, keepdims=True).astype(jnp.int32)
    place = lax.broadcasted_iota(jnp.int32, (GROUPS * cap, tokens), 0) == slot
    place = jnp.where(place, 1.0, 0.0)
    weight = weight_ref[...]
    odd = (pick_ref[...] & 1) == 1
    one = jnp.sum(jnp.where(odd, weight, 0.0), axis=1, keepdims=True)
    zero = jnp.sum(jnp.where(odd, 0.0, weight), axis=1, keepdims=True)
    lane = lax.broadcasted_iota(jnp.int32, (tokens, LANES), 1)
    value = jnp.where((lane & 1) == 1, one, zero)
    high = value.astype(bf16).astype(f32)
    extra = jnp.where(lane < 2, high, value - high).astype(bf16)
    place_b = place.astype(bf16)
    for k, ref in enumerate(out_refs):
        strip = place_b[k * cap : (k + 1) * cap]
        ref[:, :width] = mm(strip, normed).astype(bf16)
        ref[:, width:] = mm(strip, extra).astype(bf16)
    turn_ref[...] = place.T.astype(bf16)


def expand_body(*refs):
    rows, gates, ups, out_ref = refs[:8], refs[8:12], refs[12:16], refs[16]
    width = gates[0].shape[0]
    cap = rows[0].shape[0]
    part = gates[0].shape[1]
    x = jnp.concatenate([r[:, :width] for r in rows], axis=0)
    for i in range(4):
        gate = mm(x, gates[i][...])
        up = mm(x, ups[i][...])
        out_ref[:, i * part : (i + 1) * part] = (gate / (1.0 + jnp.exp(-gate)) * up).astype(bf16)


def contract_body(h_ref, d0, d1, d2, d3, *out_refs, first):
    cap = out_refs[0].shape[0]
    count = cap * len(out_refs)
    part = d0.shape[0]
    total = None
    for i, d in enumerate((d0, d1, d2, d3)):
        got = mm(h_ref[first : first + count, i * part : (i + 1) * part], d[...])
        total = got if total is None else total + got
    for k, ref in enumerate(out_refs):
        ref[...] = total[k * cap : (k + 1) * cap].astype(bf16)


def join_body(zy_ref, own_ref, other_ref, extra_ref, out_ref):
    extra = extra_ref[...].astype(f32)
    zero = extra[:, 0:1] + extra[:, 2:3]
    one = extra[:, 1:2] + extra[:, 3:4]
    odd = zy_ref[1] == 1
    mine = jnp.where(odd, one, zero)
    theirs = jnp.where(odd, zero, one)
    out_ref[...] = (own_ref[...].astype(f32) * mine + other_ref[...].astype(f32) * theirs).astype(bf16)


def restore_body(turn_ref, *refs):
    out_ref = refs[-1]
    cap = refs[0].shape[0]
    total = None
    for k, ref in enumerate(refs[:-1]):
        got = mm(turn_ref[:, k * cap : (k + 1) * cap], ref[...])
        total = got if total is None else total + got
    out_ref[...] = total.astype(bf16)


def paired_experts(moe_input, moe_gain, expert_pick, route_weight, gates, ups, downs):
    tokens, width = moe_input.shape
    ep_count = lax.axis_size("ep")
    ep_index = lax.axis_index("ep")
    cap = GROUPS * tokens // ep_count
    zy = jnp.stack([ep_index // TOPK, ep_index % TOPK]).astype(jnp.int32)

    def along(k):
        return [(i, i ^ (k * TOPK)) for i in range(ep_count)]

    across = [(i, i ^ 1) for i in range(ep_count)]
    row_type = jax.ShapeDtypeStruct((cap, width + LANES), bf16)
    wide_type = jax.ShapeDtypeStruct((cap, width), bf16)
    *sent, turn = call(
        functools.partial(route_body, cap=cap),
        "route",
        [row_type] * GROUPS + [jax.ShapeDtypeStruct((tokens, GROUPS * cap), bf16)],
        [SMEM] + [VMEM] * 5,
        32,
    )(zy, moe_input, moe_gain.reshape(1, width), expert_pick.T, expert_pick, route_weight)
    own = [sent[0]] + [lax.ppermute(sent[k], "ep", along(k)) for k in range(1, GROUPS)]
    theirs = [lax.ppermute(rows, "ep", across) for rows in own]
    part = gates[0].shape[2]
    count = 2 * GROUPS * cap
    hidden = call(
        expand_body,
        "expand",
        jax.ShapeDtypeStruct((count, 4 * part), bf16),
        [VMEM] * 16,
        48,
        flops=4 * count * width * 4 * part,
    )(*theirs, *own, *[g[0] for g in gates], *[u[0] for u in ups])
    results = [
        call(
            functools.partial(contract_body, first=i * GROUPS * cap),
            "contract",
            [wide_type] * GROUPS,
            [VMEM] * 5,
            48,
            flops=count * width * 4 * part,
        )(hidden, *[d[0] for d in downs])
        for i in range(2)
    ]
    others = [None] * GROUPS
    returned = [None] * GROUPS
    for k in (2, 3, 1, 0):
        others[k] = lax.ppermute(results[0][k], "ep", across)
    for k in (2, 3, 1, 0):
        joined = pl.pallas_call(
            join_body,
            name="join",
            out_shape=wide_type,
            grid=(1,),
            in_specs=[
                SMEM,
                pl.BlockSpec((cap, width), lambda i: (0, 0)),
                pl.BlockSpec((cap, width), lambda i: (0, 0)),
                pl.BlockSpec((cap, LANES), lambda i: (0, width // LANES)),
            ],
            out_specs=pl.BlockSpec((cap, width), lambda i: (0, 0)),
        )(zy, results[1][k], others[k], own[k])
        returned[k] = lax.ppermute(joined, "ep", along(k)) if k else joined
    return call(
        restore_body,
        "restore",
        jax.ShapeDtypeStruct((tokens, width), bf16),
        [VMEM] * (GROUPS + 1),
        32,
    )(turn, *returned)


def expand(arrived, gate_weights, up_weights):
    gate_in = jnp.einsum("necm,emf->necf", arrived, gate_weights, preferred_element_type=f32)
    up_in = jnp.einsum("necm,emf->necf", arrived, up_weights, preferred_element_type=f32)
    return (jax.nn.silu(gate_in) * up_in).astype(bf16)


def contract(hidden, down_weights):
    return jnp.einsum("necf,efm->necm", hidden, down_weights, preferred_element_type=f32)


def any_experts(moe_input, moe_gain, expert_pick, route_weight, w_gate, w_up, w_down):
    ep_count = lax.axis_size("ep")
    token_count = moe_input.shape[0]
    widened = moe_input.astype(f32)
    normed = (
        widened
        * lax.rsqrt(jnp.mean(widened * widened, axis=1, keepdims=True) + norm_eps)
        * moe_gain
    ).astype(bf16)
    local_experts = w_gate.shape[0]
    expert_total = local_experts * ep_count
    capacity = GROUPS * token_count // expert_total
    picks = expert_pick.reshape(-1)
    matches = (picks[:, None] == jnp.arange(expert_total, dtype=jnp.int32)[None, :]).astype(
        jnp.int32
    )
    ranks = jnp.sum((jnp.cumsum(matches, axis=0) - matches) * matches, axis=1)
    slots = picks * capacity + ranks
    owners = jnp.arange(picks.shape[0], dtype=jnp.int32) // TOPK
    table = jnp.full((expert_total * capacity,), token_count, jnp.int32).at[slots].set(owners)
    padded = jnp.concatenate([normed, jnp.zeros((1, normed.shape[1]), bf16)], axis=0)
    outgoing = padded[table].reshape(ep_count, local_experts, capacity, normed.shape[1])
    arrived = lax.all_to_all(outgoing, "ep", split_axis=0, concat_axis=0, tiled=True)
    gate_all, up_all, down_all = (
        lax.all_gather(w_gate, "tp", axis=2, tiled=True),
        lax.all_gather(w_up, "tp", axis=2, tiled=True),
        lax.all_gather(w_down, "tp", axis=1, tiled=True),
    )
    served = contract(expand(arrived, gate_all, up_all), down_all).astype(bf16)
    returned = lax.all_to_all(served, "ep", split_axis=0, concat_axis=0, tiled=True)
    flat = returned.reshape(expert_total * capacity, returned.shape[3])
    chosen = flat[slots].reshape(token_count, TOPK, flat.shape[1]).astype(f32)
    return jnp.sum(chosen * route_weight[:, :, None], axis=1).astype(bf16)


def local(
    query_rows,
    key_rows,
    value_rows,
    key_bias,
    out_weight,
    moe_input,
    moe_gain,
    expert_pick,
    route_weight,
    w_gate,
    w_up,
    w_down,
):
    tp_size = lax.axis_size("tp")
    ep_count = lax.axis_size("ep")
    paired = w_gate.shape[0] == 1 and ep_count == GROUPS * TOPK
    if paired:
        gates = spread(w_gate, tp_size)
        ups = spread(w_up, tp_size)
        downs = spread(w_down, tp_size)
    out_pieces = spread(out_weight, tp_size)
    mixer_out = mixer(query_rows, key_rows, value_rows, key_bias, out_pieces)
    if paired:
        routed_out = paired_experts(
            moe_input, moe_gain, expert_pick, route_weight, gates, ups, downs
        )
    else:
        routed_out = any_experts(
            moe_input, moe_gain, expert_pick, route_weight, w_gate, w_up, w_down
        )
    return (mixer_out, routed_out)


def solution(mesh):
    placed = (
        P("ep", "tp"),
        P("ep", "tp"),
        P("ep", "tp"),
        P(None, "tp"),
        P("tp", None),
        P(("ep", "tp"), None),
        P(),
        P(("ep", "tp"), None),
        P(("ep", "tp"), None),
        P("ep", None, "tp"),
        P("ep", None, "tp"),
        P("ep", "tp", None),
    )
    return jax.shard_map(
        local,
        mesh=mesh,
        in_specs=placed,
        out_specs=(P(("ep", "tp"), None), P(("ep", "tp"), None)),
        check_vma=False,
    )
```

```python
import functools
import math

import jax
import jax.numpy as jnp
from jax import lax
from jax.experimental import pallas as pl
from jax.experimental.pallas import tpu as pltpu
from jax.sharding import PartitionSpec as P


HEAD_DIM = 64
GROUPS = 4
TOPK = 2
LANES = 128
KEY_TILE = 256
LOG2E = math.log2(math.e)
MIB = 1 << 20

norm_eps = 1e-06
bf16 = jnp.bfloat16
f32 = jnp.float32

RETURN_ORDER = (2, 3, 1, 0)

VMEM = pl.BlockSpec(memory_space=pltpu.VMEM)


def whole(array):
    return pl.BlockSpec(array.shape, lambda i: (0,) * array.ndim)


def call(body, outs, ins, limit, flops=0, moved=0, scratch=()):
    return pl.pallas_call(
        body,
        out_shape=outs,
        scratch_shapes=scratch,
        grid=(1,),
        in_specs=ins,
        out_specs=jax.tree.map(lambda _: VMEM, outs),
        compiler_params=pltpu.CompilerParams(vmem_limit_bytes=limit * MIB),
        cost_estimate=pl.CostEstimate(flops=flops, bytes_accessed=moved, transcendentals=0),
    )


def exchange(piece, axes):
    return lax.all_to_all(piece, axes, split_axis=0, concat_axis=0, tiled=True)


def spot_of(sharers):
    ep = lax.axis_index("ep")
    return lax.rem(ep, sharers), lax.axis_index("tp"), lax.div(ep, sharers)


def mm(a, b):
    return jnp.dot(a, b, preferred_element_type=f32)


def pack_body(bias_any, q_ref, k_ref, v_ref, bias_ref, out_ref, *, heads, sharers, parts):
    bias_into(bias_any, bias_ref, spot_of(sharers)[2])
    rows = q_ref.shape[0]
    part_rows = rows // parts
    sub = part_rows // sharers
    half = rows // sharers // 2
    for h in range(heads):
        cols = pl.ds(h * HEAD_DIM, HEAD_DIM)
        pair = jnp.concatenate([k_ref[:, cols], v_ref[:, cols]], axis=1)
        for s in range(sharers):
            out_ref[h * sharers + s, :rows] = pair
            mine = jnp.concatenate(
                [q_ref[pl.ds(t * part_rows + s * sub, sub), cols] for t in range(parts)], axis=0
            )
            out_ref[h * sharers + s, rows:] = jnp.concatenate([mine[:half], mine[half:]], axis=1)


def bias_into(bias_any, out_ref, head):
    tiles, width = out_ref.shape
    line = bias_any[pl.ds(head, 1)] * LOG2E
    for i in range(tiles):
        out_ref[i : i + 1] = line[:, i * width : (i + 1) * width]


def pack_pair_body(bias_any, q_ref, k_ref, v_ref, bias_ref, *refs, heads, parts):
    out_refs, all_ref = refs[:-1], refs[-1]
    share, _, head = spot_of(TOPK)
    bias_into(bias_any, bias_ref, head)
    rows = q_ref.shape[0]
    part_rows = rows // parts
    sub = part_rows // TOPK
    half = rows // TOPK // 2
    second = share == 1
    for h in range(heads):
        cols = pl.ds(h * HEAD_DIM, HEAD_DIM)
        packed = []
        for s in range(TOPK):
            mine = jnp.concatenate(
                [q_ref[pl.ds(t * part_rows + s * sub, sub), cols] for t in range(parts)], axis=0
            )
            packed.append(jnp.concatenate([mine[:half], mine[half:]], axis=1))
        all_ref[h, :half] = jnp.where(second, packed[1], packed[0])
        all_ref[h, half : half + rows] = jnp.concatenate([k_ref[:, cols], v_ref[:, cols]], axis=1)
        all_ref[h, half + rows :] = jnp.where(second, packed[0], packed[1])
    for k, ref in enumerate(out_refs):
        ref[...] = all_ref[head ^ k]


def attend_pair_body(bias_ref, *refs, rows, sub, parts):
    arrived, out_refs = refs[: 2 * GROUPS], refs[2 * GROUPS : 3 * GROUPS]
    got_ref, *scratch = refs[3 * GROUPS :]
    half = sub * parts // 2
    y, _, z = spot_of(TOPK)
    for k in range(GROUPS):
        for side in range(2):
            ref = arrived[side * GROUPS + k]
            block = (z ^ k) * TOPK + (y ^ side)
            got_ref[block, :rows] = ref[half : half + rows]
            got_ref[block, rows:] = ref[half + rows :] if side else ref[:half]
    attend_body(got_ref, bias_ref, *out_refs, *scratch, rows=rows, sub=sub, parts=parts)


def attend_body(got_ref, bias_ref, *refs, rows, sub, parts):
    (*out_refs, acc_ref, run_ref, gap_ref, rest_ref, soft_ref, weight_ref, sum_ref, all_ref) = refs
    blocks = got_ref.shape[0]
    mine = sub * parts
    half = mine // 2
    share = spot_of(rows // mine)[0]
    scale = HEAD_DIM**-0.5 * LOG2E
    tiles = rows // KEY_TILE
    part_rows = rows // parts
    low = lax.broadcasted_iota(jnp.int32, (half, LANES), 1) < HEAD_DIM
    later = (
        lax.broadcasted_iota(jnp.int32, (KEY_TILE, KEY_TILE), 0)
        > lax.broadcasted_iota(jnp.int32, (KEY_TILE, KEY_TILE), 1)
    )
    after = jnp.where(later, 1.0, 0.0).astype(bf16)
    every = jnp.ones((KEY_TILE, KEY_TILE), bf16)

    def cut(c):
        return slice(c * KEY_TILE, (c + 1) * KEY_TILE)

    def query_of(b):
        packed = got_ref[b, pl.ds(rows, half)].astype(f32)
        return jnp.concatenate(
            [
                jnp.where(low, packed, 0.0),
                jnp.where(low, pltpu.roll(packed, HEAD_DIM, 1), 0.0),
            ],
            axis=0,
        ).astype(bf16)

    def causal(c):
        row = lax.broadcasted_iota(jnp.int32, (mine, KEY_TILE), 0)
        spot = row + share * sub
        for t in range(1, parts):
            spot = spot + jnp.where(row >= t * sub, part_rows - sub, 0)
        return lax.broadcasted_iota(jnp.int32, (mine, KEY_TILE), 1) + c * KEY_TILE < spot

    def soften(b, source, p, masked):
        query = query_of(b)
        for c in reversed(range(tiles)):
            raw = lax.dot_general(
                query,
                got_ref[source, cut(c)],
                (((1,), (1,)), ((), ())),
                preferred_element_type=f32,
            )
            score = raw * scale + bias_ref[pl.ds(source * tiles + c, 1)]
            soft = lax.log2(1.0 + jnp.exp2(jnp.minimum(score, 126.0)))
            soft = jnp.maximum(score, soft)
            gap = score - soft
            if masked:
                keep = causal(c)
                soft = jnp.where(keep, soft, 0.0)
                gap = jnp.where(keep, gap, -1e30)
            gap_ref[p, :, cut(c)] = gap
            soft_ref[p, :, cut(c)] = soft.astype(bf16)

    def total_up(p):
        for c in reversed(range(tiles)):
            rest = mm(soft_ref[p, :, cut(c)], after)
            for later_c in range(c + 1, tiles):
                rest = rest + mm(soft_ref[p, :, cut(later_c)], every)
            rest_ref[p, :, cut(c)] = rest
            if c == 0:
                sum_ref[p] = rest[:, :LANES] + soft_ref[p, :, :LANES].astype(f32)

    def weigh(p):
        for c in range(tiles):
            weight = jnp.exp2(gap_ref[p, :, cut(c)] - rest_ref[p, :, cut(c)])
            weight_ref[p, :, cut(c)] = weight.astype(bf16)
        all_ref[p] = jnp.broadcast_to(sum_ref[p, :, :1], (mine, LANES))

    def gather(b, source, p, valid, fresh):
        portion = mm(weight_ref[p], got_ref[source, :rows])
        total = all_ref[p]
        if fresh:
            acc = portion
            run = total
        else:
            run = run_ref[b]
            acc = acc_ref[b] + portion * jnp.exp2(-run)
            run = run + total
        acc_ref[b] = jnp.where(valid, acc, acc_ref[b])
        run_ref[b] = jnp.where(valid, run, run_ref[b])

    def diagonal(k, _):
        for p in range(2):
            i = 2 * k + p
            old = jnp.minimum(jnp.maximum(i - 3, 0), blocks - 1)
            now = jnp.minimum(i, blocks - 1)
            gather(old, old, 1 - p, (i >= 3) & (i < blocks + 3), True)
            weigh(p)
            total_up(1 - p)
            soften(now, now, p, True)
        return 0

    lax.fori_loop(0, (blocks + 4) // 2, diagonal, 0)
    count = blocks * (blocks - 1) // 2

    def step(k, state):
        for p in range(2):
            i = 2 * k + p
            gather(*state[0:2], 1 - p, (i >= 3) & (i < count + 3), False)
            weigh(p)
            total_up(1 - p)
            b, source = state[6:8]
            soften(b, source, p, False)
            wrap = source == 0
            more = i + 1 < count
            b_next = jnp.where(more, jnp.where(wrap, b + 1, b), b)
            next_source = jnp.where(more, jnp.where(wrap, b, source - 1), source)
            state = (*state[2:], b_next, next_source)
        return state

    if count > 0:
        lax.fori_loop(0, (count + 4) // 2, step, (jnp.int32(1), jnp.int32(0)) * 4)

    few = sub // 2
    keep = lax.broadcasted_iota(jnp.int32, (few, LANES), 1) < HEAD_DIM

    def finish(b, out_at):
        acc = acc_ref[b]
        turned = pltpu.roll(acc, HEAD_DIM, 1)
        for t in range(parts):
            left = turned[t * sub : t * sub + few]
            right = acc[t * sub + few : (t + 1) * sub]
            out_at[t] = jnp.where(keep, left, right).astype(bf16)

    if len(out_refs) > 1:
        for k, ref in enumerate(out_refs):
            for side in range(TOPK):
                finish(lax.axis_index("ep") ^ (k * TOPK + side), ref.at[side])
    else:

        def each(b, _):
            finish(b, out_refs[0].at[b])
            return 0

        lax.fori_loop(0, blocks, each, 0)


def project_with(source, weights, out_ref, *, few, heads, sharers):
    low = lax.broadcasted_iota(jnp.int32, (few, LANES), 1) < HEAD_DIM
    total = None
    for m, w_ref in enumerate(weights):
        strips = []
        for s in range(sharers):
            firsts, seconds = [], []
            for h in range(0, heads, 2):
                a = source(m, h * sharers + s).astype(f32)
                b = source(m, (h + 1) * sharers + s).astype(f32)
                firsts.append(jnp.where(low, a, pltpu.roll(b, HEAD_DIM, 1)))
                seconds.append(jnp.where(low, pltpu.roll(a, HEAD_DIM, 1), b))
            strips.append(jnp.concatenate(firsts, axis=1))
            strips.append(jnp.concatenate(seconds, axis=1))
        left = jnp.concatenate(strips, axis=0).astype(bf16)
        part = mm(left, w_ref[...])
        total = part if total is None else total + part
    out_ref[...] = total.astype(bf16)


def project_body(got_ref, *refs, heads, sharers, parts):
    here = lax.axis_index("tp")
    project_with(
        lambda m, ep: got_ref[ep * parts + (here ^ m)],
        refs[:-1],
        refs[-1],
        few=got_ref.shape[1],
        heads=heads,
        sharers=sharers,
    )


def sides_body(*refs):
    sources, (kept, given) = refs[:GROUPS], refs[GROUPS:]
    for k, source in enumerate(sources):
        kept[k] = source[0]
        given[k] = source[1]


def parts_body(kept, given, *outs):
    here = lax.axis_index("tp")
    for m, out in enumerate(outs):
        for k in range(GROUPS):
            for side, source in enumerate((kept, given)):
                out[k * TOPK + side] = source[k, here ^ m]


def project_pair_body(*refs, heads):
    here = lax.axis_index("ep")
    sources = refs[:4]
    project_with(
        lambda m, ep: sources[m][here ^ ep],
        refs[4:8],
        refs[8],
        few=sources[0].shape[1],
        heads=heads,
        sharers=TOPK,
    )


def stage_body(*refs):
    half = len(refs) // 2
    for a, b in zip(refs[:half], refs[half:]):
        b[...] = a[...]


def spread(piece, size):
    cross = [(i, i ^ 2) for i in range(size)]
    beside = [(i, i ^ 1) for i in range(size)]
    far = lax.ppermute(piece, "tp", cross)
    near = lax.ppermute(piece, "tp", beside)
    return (piece, near, far, lax.ppermute(far, "tp", beside))


def mixer(query_rows, key_rows, value_rows, key_bias, out_pieces, paired):
    rows = query_rows.shape[0]
    heads = query_rows.shape[1] // HEAD_DIM
    ep_count = lax.axis_size("ep")
    parts = lax.axis_size("tp")
    sharers = ep_count // heads
    sub = rows // parts // sharers
    mine = sub * parts
    tall = rows + mine // 2
    bias_type = jax.ShapeDtypeStruct((key_bias.shape[0] // KEY_TILE, KEY_TILE), f32)
    attend_type = jax.ShapeDtypeStruct((ep_count, parts, sub // 2, LANES), bf16)
    work = 3 * ep_count * ep_count * mine * rows * LANES
    scratch = [
        pltpu.VMEM((ep_count, mine, LANES), f32),
        pltpu.VMEM((ep_count, mine, LANES), f32),
        pltpu.VMEM((2, mine, rows), f32),
        pltpu.VMEM((2, mine, rows), f32),
        pltpu.VMEM((2, mine, rows), bf16),
        pltpu.VMEM((2, mine, rows), bf16),
        pltpu.VMEM((2, mine, LANES), f32),
        pltpu.VMEM((2, mine, LANES), f32),
    ]
    sizes = {"rows": rows, "sub": sub, "parts": parts}
    if paired:
        bias, *packed = call(
            functools.partial(pack_pair_body, heads=heads, parts=parts),
            [bias_type] + [jax.ShapeDtypeStruct((tall + mine // 2, LANES), bf16)] * GROUPS,
            [whole(key_bias.T)] + [whole(query_rows)] * 3,
            12,
            scratch=[pltpu.VMEM((heads, tall + mine // 2, LANES), bf16)],
        )(key_bias.T, query_rows, key_rows, value_rows)
        own = [packed[0]]
        for k in range(1, GROUPS):
            pairs = [(i, i ^ (k * TOPK)) for i in range(ep_count)]
            own.append(lax.ppermute(packed[k], "ep", pairs))
        across = [(i, i ^ 1) for i in range(ep_count)]
        theirs = [lax.ppermute(piece, "ep", across) for piece in own]
        block = (parts, sub // 2, LANES)
        attended = call(
            functools.partial(attend_pair_body, **sizes),
            [jax.ShapeDtypeStruct((TOPK, *block), bf16)] * GROUPS,
            [VMEM] * (1 + 2 * GROUPS),
            16,
            flops=work,
            scratch=[pltpu.VMEM((ep_count, tall, LANES), bf16)] + scratch,
        )(bias, *own, *theirs)
        attended = list(attended)
        for k in range(1, GROUPS):
            pairs = [(i, i ^ (k * TOPK)) for i in range(ep_count)]
            attended[k] = lax.ppermute(attended[k], "ep", pairs)
        side_type = jax.ShapeDtypeStruct((GROUPS, *block), bf16)
        kept, given = call(sides_body, [side_type] * 2, [VMEM] * GROUPS, 4)(*attended)
        given = lax.ppermute(given, "ep", across)
        by_part = call(
            parts_body,
            [jax.ShapeDtypeStruct((ep_count, sub // 2, LANES), bf16)] * parts,
            [VMEM] * 2,
            4,
        )(kept, given)
        by_part = list(by_part)
        for m in range(1, parts):
            pairs = [(i, i ^ m) for i in range(parts)]
            by_part[m] = lax.ppermute(by_part[m], "tp", pairs)
        return call(
            functools.partial(project_pair_body, heads=heads),
            jax.ShapeDtypeStruct((rows // parts, out_pieces[0].shape[1]), bf16),
            [VMEM] * 8,
            12,
            flops=2 * rows * heads * HEAD_DIM * out_pieces[0].shape[1],
        )(*by_part, *out_pieces)
    else:
        bias, outgoing = call(
            functools.partial(pack_body, heads=heads, sharers=sharers, parts=parts),
            [bias_type, jax.ShapeDtypeStruct((ep_count, tall, LANES), bf16)],
            [whole(key_bias.T)] + [whole(query_rows)] * 3,
            12,
        )(key_bias.T, query_rows, key_rows, value_rows)
        got = exchange(outgoing, "ep")
        attended = call(
            functools.partial(attend_body, **sizes),
            attend_type,
            [VMEM, VMEM],
            16,
            flops=work,
            scratch=scratch,
        )(got, bias)
    attended = attended.reshape(ep_count * parts, sub // 2, LANES)
    back = exchange(attended, ("ep", "tp"))
    return call(
        functools.partial(project_body, heads=heads, sharers=sharers, parts=parts),
        jax.ShapeDtypeStruct((rows // parts, out_pieces[0].shape[1]), bf16),
        [VMEM] * 5,
        12,
        flops=2 * rows * heads * HEAD_DIM * out_pieces[0].shape[1],
    )(back, *out_pieces)


def route_body(x_ref, gain_ref, pick_ref, weight_ref, *outs, cap):
    out_refs, turn_ref = outs[:GROUPS], outs[GROUPS]
    tokens, width = x_ref.shape
    z = spot_of(TOPK)[2]
    pick = pick_ref[...]
    lanes = GROUPS * 2
    group = lax.broadcasted_iota(jnp.int32, (lanes, tokens), 0)
    inside = (pick[0:1] >= group * TOPK) & (pick[0:1] < (group + 1) * TOPK)
    match = jnp.where(inside, 1.0, 0.0)
    before = (
        lax.broadcasted_iota(jnp.int32, (tokens, tokens), 0)
        < lax.broadcasted_iota(jnp.int32, (tokens, tokens), 1)
    )
    rank = mm(match.astype(bf16), jnp.where(before, 1.0, 0.0).astype(bf16))
    first = ((group ^ z) * cap).astype(f32)
    slot = jnp.sum(match * (rank + first), axis=0, keepdims=True).astype(jnp.int32)
    place = lax.broadcasted_iota(jnp.int32, (GROUPS * cap, tokens), 0) == slot
    place = jnp.where(place, 1.0, 0.0)
    weight = weight_ref[...]
    odd = (pick & 1) == 1
    one = jnp.sum(jnp.where(odd, weight, 0.0), axis=0, keepdims=True)
    zero = jnp.sum(jnp.where(odd, 0.0, weight), axis=0, keepdims=True)
    line = lax.broadcasted_iota(jnp.int32, (LANES, tokens), 0)
    value = jnp.where((line & 1) == 1, one, zero)
    high = value.astype(bf16).astype(f32)
    extra = jnp.where(line < 2, high, value - high).astype(bf16)
    place_b = place.astype(bf16)
    turn_ref[...] = place.T.astype(bf16)
    wide = x_ref[...].astype(f32)
    normed = (
        wide
        * lax.rsqrt(jnp.mean(wide * wide, axis=1, keepdims=True) + norm_eps)
        * gain_ref[...]
    ).astype(bf16)
    for k, ref in enumerate(out_refs):
        strip = place_b[k * cap : (k + 1) * cap]
        ref[:, :width] = mm(strip, normed).astype(bf16)
        ref[:, width:] = lax.dot_general(
            strip, extra, (((1,), (1,)), ((), ())), preferred_element_type=f32
        ).astype(bf16)


def expand_body(*refs):
    rows, gates, ups = refs[:GROUPS], refs[GROUPS : GROUPS + 4], refs[GROUPS + 4 : GROUPS + 8]
    out_ref, mix_ref = refs[GROUPS + 8 :]
    width, part = gates[0].shape
    x = jnp.concatenate([r[:, :width] for r in rows], axis=0)
    mix_ref[...] = jnp.concatenate([r[:, width:] for r in rows], axis=0)
    for i in range(4):
        gate = mm(x, gates[i][...])
        up = mm(x, ups[i][...])
        out_ref[:, i * part : (i + 1) * part] = (gate / (1.0 + jnp.exp(-gate)) * up).astype(bf16)


def contract_body(h_ref, d0, d1, d2, d3, *out_refs):
    cap = out_refs[0].shape[0]
    part = d0.shape[0]
    total = None
    for i, d in enumerate((d0, d1, d2, d3)):
        got = mm(h_ref[:, i * part : (i + 1) * part], d[...])
        total = got if total is None else total + got
    for k, ref in enumerate(out_refs):
        ref[...] = total[k * cap : (k + 1) * cap].astype(bf16)


def join_body(own_ref, other_ref, mix_ref, out_ref, *, first):
    extra = mix_ref[first : first + own_ref.shape[0]].astype(f32)
    zero = extra[:, 0:1] + extra[:, 2:3]
    one = extra[:, 1:2] + extra[:, 3:4]
    odd = spot_of(TOPK)[0] == 1
    mine = jnp.where(odd, one, zero)
    theirs = jnp.where(odd, zero, one)
    out_ref[...] = (own_ref[...].astype(f32) * mine + other_ref[...].astype(f32) * theirs).astype(bf16)


def restore_body(turn_ref, *refs):
    out_ref = refs[-1]
    cap = refs[0].shape[0]
    total = None
    for k, ref in enumerate(refs[:-1]):
        got = mm(turn_ref[:, k * cap : (k + 1) * cap], ref[...])
        total = got if total is None else total + got
    out_ref[...] = total.astype(bf16)


def paired_experts(moe_input, moe_gain, expert_pick, route_weight, gates, ups, downs):
    tokens, width = moe_input.shape
    ep_count = lax.axis_size("ep")
    cap = GROUPS * tokens // ep_count

    def along(k):
        return [(i, i ^ (k * TOPK)) for i in range(ep_count)]

    across = [(i, i ^ 1) for i in range(ep_count)]
    row_type = jax.ShapeDtypeStruct((cap, width + LANES), bf16)
    wide_type = jax.ShapeDtypeStruct((cap, width), bf16)
    route_args = (moe_input, moe_gain.reshape(1, width), expert_pick.T, route_weight.T)
    *sent, turn = call(
        functools.partial(route_body, cap=cap),
        [row_type] * GROUPS + [jax.ShapeDtypeStruct((tokens, GROUPS * cap), bf16)],
        [whole(a) for a in route_args],
        12,
    )(*route_args)
    own = [sent[0]] + [lax.ppermute(sent[k], "ep", along(k)) for k in range(1, GROUPS)]
    theirs = [lax.ppermute(rows, "ep", across) for rows in own]
    part = gates[0].shape[2]
    count = GROUPS * cap
    gates = [g[0] for g in gates]
    ups = [u[0] for u in ups]
    piece_type = jax.ShapeDtypeStruct(gates[0].shape, bf16)
    gates[0], ups[0] = call(stage_body, [piece_type] * 2, [VMEM] * 2, 8)(gates[0], ups[0])
    results = {}
    for side, rows in (("a", own), ("b", theirs)):
        hidden, got = call(
            expand_body,
            [
                jax.ShapeDtypeStruct((count, 4 * part), bf16),
                jax.ShapeDtypeStruct((count, LANES), bf16),
            ],
            [VMEM] * (GROUPS + 8),
            16,
            flops=4 * count * width * 4 * part,
        )(*rows, *gates, *ups)
        if side == "a":
            mix = got
        results[side] = call(
            contract_body, [wide_type] * GROUPS, [VMEM] * 5, 16, flops=2 * count * width * 4 * part
        )(hidden, *[d[0] for d in downs])
    others = [None] * GROUPS
    returned = [None] * GROUPS
    for k in RETURN_ORDER:
        others[k] = lax.ppermute(results["b"][k], "ep", across)
    for k in RETURN_ORDER:
        joined = call(
            functools.partial(join_body, first=k * cap), wide_type, [VMEM] * 3, 4
        )(results["a"][k], others[k], mix)
        returned[k] = lax.ppermute(joined, "ep", along(k)) if k else joined
    return call(
        restore_body, jax.ShapeDtypeStruct((tokens, width), bf16), [VMEM] * (GROUPS + 1), 8
    )(turn, *returned)


def expand(arrived, gate_weights, up_weights):
    gate_in = jnp.einsum("necm,emf->necf", arrived, gate_weights, preferred_element_type=f32)
    up_in = jnp.einsum("necm,emf->necf", arrived, up_weights, preferred_element_type=f32)
    return (jax.nn.silu(gate_in) * up_in).astype(bf16)


def contract(hidden, down_weights):
    return jnp.einsum("necf,efm->necm", hidden, down_weights, preferred_element_type=f32)


def any_experts(moe_input, moe_gain, expert_pick, route_weight, w_gate, w_up, w_down):
    ep_count = lax.axis_size("ep")
    token_count = moe_input.shape[0]
    widened = moe_input.astype(f32)
    normed = (
        widened
        * lax.rsqrt(jnp.mean(widened * widened, axis=1, keepdims=True) + norm_eps)
        * moe_gain
    ).astype(bf16)
    local_experts = w_gate.shape[0]
    expert_total = local_experts * ep_count
    capacity = GROUPS * token_count // expert_total
    picks = expert_pick.reshape(-1)
    matches = (picks[:, None] == jnp.arange(expert_total, dtype=jnp.int32)[None, :]).astype(
        jnp.int32
    )
    ranks = jnp.sum((jnp.cumsum(matches, axis=0) - matches) * matches, axis=1)
    slots = picks * capacity + ranks
    owners = jnp.arange(picks.shape[0], dtype=jnp.int32) // TOPK
    table = jnp.full((expert_total * capacity,), token_count, jnp.int32).at[slots].set(owners)
    padded = jnp.concatenate([normed, jnp.zeros((1, normed.shape[1]), bf16)], axis=0)
    outgoing = padded[table].reshape(ep_count, local_experts, capacity, normed.shape[1])
    arrived = lax.all_to_all(outgoing, "ep", split_axis=0, concat_axis=0, tiled=True)
    gate_all, up_all, down_all = (
        lax.all_gather(w_gate, "tp", axis=2, tiled=True),
        lax.all_gather(w_up, "tp", axis=2, tiled=True),
        lax.all_gather(w_down, "tp", axis=1, tiled=True),
    )
    served = contract(expand(arrived, gate_all, up_all), down_all).astype(bf16)
    returned = lax.all_to_all(served, "ep", split_axis=0, concat_axis=0, tiled=True)
    flat = returned.reshape(expert_total * capacity, returned.shape[3])
    chosen = flat[slots].reshape(token_count, TOPK, flat.shape[1]).astype(f32)
    return jnp.sum(chosen * route_weight[:, :, None], axis=1).astype(bf16)


def local(
    query_rows,
    key_rows,
    value_rows,
    key_bias,
    out_weight,
    moe_input,
    moe_gain,
    expert_pick,
    route_weight,
    w_gate,
    w_up,
    w_down,
):
    tp_size = lax.axis_size("tp")
    paired = is_paired(lax.axis_size("ep"), w_gate.shape[0])
    paired = paired and query_rows.shape[1] == GROUPS * HEAD_DIM
    if paired:
        gates = spread(w_gate, tp_size)
        ups = spread(w_up, tp_size)
        downs = spread(w_down, tp_size)
        routed_out = paired_experts(
            moe_input, moe_gain, expert_pick, route_weight, gates, ups, downs
        )
    else:
        routed_out = any_experts(
            moe_input, moe_gain, expert_pick, route_weight, w_gate, w_up, w_down
        )
    out_pieces = spread(out_weight, tp_size)
    mixer_out = mixer(query_rows, key_rows, value_rows, key_bias, out_pieces, paired)
    return (mixer_out, routed_out)


def is_paired(ep_count, local_experts):
    return local_experts == 1 and ep_count == GROUPS * TOPK


def solution(mesh):
    placed = (
        P("ep", "tp"),
        P("ep", "tp"),
        P("ep", "tp"),
        P(None, "tp"),
        P("tp", None),
        P(("ep", "tp"), None),
        P(),
        P(("ep", "tp"), None),
        P(("ep", "tp"), None),
        P("ep", None, "tp"),
        P("ep", None, "tp"),
        P("ep", "tp", None),
    )
    return jax.shard_map(
        local,
        mesh=mesh,
        in_specs=placed,
        out_specs=(P(("ep", "tp"), None), P(("ep", "tp"), None)),
        check_vma=False,
    )
```

```python
import functools
import math

import jax
import jax.numpy as jnp
from jax import lax
from jax.experimental import pallas as pl
from jax.experimental.pallas import tpu as pltpu
from jax.sharding import PartitionSpec as P


HEAD_DIM = 64
GROUPS = 4
TOPK = 2
LANES = 128
KEY_TILE = 256
LOG2E = math.log2(math.e)
MIB = 1 << 20

norm_eps = 1e-06
bf16 = jnp.bfloat16
f32 = jnp.float32

RETURN_ORDER = (2, 4, 1, 3, 0)

VMEM = pl.BlockSpec(memory_space=pltpu.VMEM)


def whole(array):
    return pl.BlockSpec(array.shape, lambda i: (0,) * array.ndim)


def call(body, outs, ins, limit, flops=0, moved=0, scratch=()):
    return pl.pallas_call(
        body,
        out_shape=outs,
        scratch_shapes=scratch,
        grid=(1,),
        in_specs=ins,
        out_specs=jax.tree.map(lambda _: VMEM, outs),
        compiler_params=pltpu.CompilerParams(vmem_limit_bytes=limit * MIB),
        cost_estimate=pl.CostEstimate(flops=flops, bytes_accessed=moved, transcendentals=0),
    )


def exchange(piece, axes):
    return lax.all_to_all(piece, axes, split_axis=0, concat_axis=0, tiled=True)


def spot_of(sharers):
    ep = lax.axis_index("ep")
    return lax.rem(ep, sharers), lax.axis_index("tp"), lax.div(ep, sharers)


def mm(a, b):
    return jnp.dot(a, b, preferred_element_type=f32)


def pack_body(bias_any, q_ref, k_ref, v_ref, bias_ref, out_ref, *, heads, sharers, parts):
    bias_into(bias_any, bias_ref, spot_of(sharers)[2])
    rows = q_ref.shape[0]
    part_rows = rows // parts
    sub = part_rows // sharers
    half = rows // sharers // 2
    for h in range(heads):
        cols = pl.ds(h * HEAD_DIM, HEAD_DIM)
        pair = jnp.concatenate([k_ref[:, cols], v_ref[:, cols]], axis=1)
        for s in range(sharers):
            out_ref[h * sharers + s, :rows] = pair
            mine = jnp.concatenate(
                [q_ref[pl.ds(t * part_rows + s * sub, sub), cols] for t in range(parts)], axis=0
            )
            out_ref[h * sharers + s, rows:] = jnp.concatenate([mine[:half], mine[half:]], axis=1)


def bias_into(bias_any, out_ref, head):
    tiles, width = out_ref.shape
    line = bias_any[pl.ds(head, 1)] * LOG2E
    for i in range(tiles):
        out_ref[i : i + 1] = line[:, i * width : (i + 1) * width]


def pack_pair_body(bias_any, q_ref, k_ref, v_ref, bias_ref, *refs, heads, parts):
    out_refs, all_ref = refs[:-1], refs[-1]
    share, _, head = spot_of(TOPK)
    bias_into(bias_any, bias_ref, head)
    rows = q_ref.shape[0]
    part_rows = rows // parts
    sub = part_rows // TOPK
    half = rows // TOPK // 2
    second = share == 1
    for h in range(heads):
        cols = pl.ds(h * HEAD_DIM, HEAD_DIM)
        packed = []
        for s in range(TOPK):
            mine = jnp.concatenate(
                [q_ref[pl.ds(t * part_rows + s * sub, sub), cols] for t in range(parts)], axis=0
            )
            packed.append(jnp.concatenate([mine[:half], mine[half:]], axis=1))
        all_ref[h, :half] = jnp.where(second, packed[1], packed[0])
        all_ref[h, half : half + rows] = jnp.concatenate([k_ref[:, cols], v_ref[:, cols]], axis=1)
        all_ref[h, half + rows :] = jnp.where(second, packed[0], packed[1])
    for k, ref in enumerate(out_refs):
        ref[...] = all_ref[head ^ k]


def attend_pair_body(bias_ref, *refs, rows, sub, parts):
    arrived, out_refs = refs[: 2 * GROUPS], refs[2 * GROUPS : 3 * GROUPS]
    got_ref, *scratch = refs[3 * GROUPS :]
    half = sub * parts // 2
    y, _, z = spot_of(TOPK)
    for k in range(GROUPS):
        for side in range(2):
            ref = arrived[side * GROUPS + k]
            block = (z ^ k) * TOPK + (y ^ side)
            got_ref[block, :rows] = ref[half : half + rows]
            got_ref[block, rows:] = ref[half + rows :] if side else ref[:half]
    attend_body(got_ref, bias_ref, *out_refs, *scratch, rows=rows, sub=sub, parts=parts)


def attend_body(got_ref, bias_ref, *refs, rows, sub, parts):
    (*out_refs, acc_ref, run_ref, gap_ref, rest_ref, soft_ref, weight_ref, sum_ref, all_ref) = refs
    blocks = got_ref.shape[0]
    mine = sub * parts
    half = mine // 2
    share = spot_of(rows // mine)[0]
    scale = HEAD_DIM**-0.5 * LOG2E
    tiles = rows // KEY_TILE
    part_rows = rows // parts
    low = lax.broadcasted_iota(jnp.int32, (half, LANES), 1) < HEAD_DIM
    later = (
        lax.broadcasted_iota(jnp.int32, (KEY_TILE, KEY_TILE), 0)
        > lax.broadcasted_iota(jnp.int32, (KEY_TILE, KEY_TILE), 1)
    )
    after = jnp.where(later, 1.0, 0.0).astype(bf16)
    every = jnp.ones((KEY_TILE, KEY_TILE), bf16)

    def cut(c):
        return slice(c * KEY_TILE, (c + 1) * KEY_TILE)

    def query_of(b):
        packed = got_ref[b, pl.ds(rows, half)].astype(f32)
        return jnp.concatenate(
            [
                jnp.where(low, packed, 0.0),
                jnp.where(low, pltpu.roll(packed, HEAD_DIM, 1), 0.0),
            ],
            axis=0,
        ).astype(bf16)

    def causal(c):
        row = lax.broadcasted_iota(jnp.int32, (mine, KEY_TILE), 0)
        spot = row + share * sub
        for t in range(1, parts):
            spot = spot + jnp.where(row >= t * sub, part_rows - sub, 0)
        return lax.broadcasted_iota(jnp.int32, (mine, KEY_TILE), 1) + c * KEY_TILE < spot

    def soften(b, source, p, masked):
        query = query_of(b)
        for c in reversed(range(tiles)):
            raw = lax.dot_general(
                query,
                got_ref[source, cut(c)],
                (((1,), (1,)), ((), ())),
                preferred_element_type=f32,
            )
            score = raw * scale + bias_ref[pl.ds(source * tiles + c, 1)]
            soft = lax.log2(1.0 + jnp.exp2(jnp.minimum(score, 126.0)))
            soft = jnp.maximum(score, soft)
            gap = score - soft
            if masked:
                keep = causal(c)
                soft = jnp.where(keep, soft, 0.0)
                gap = jnp.where(keep, gap, -1e30)
            gap_ref[p, :, cut(c)] = gap
            soft_ref[p, :, cut(c)] = soft.astype(bf16)

    def total_up(p):
        for c in reversed(range(tiles)):
            rest = mm(soft_ref[p, :, cut(c)], after)
            for later_c in range(c + 1, tiles):
                rest = rest + mm(soft_ref[p, :, cut(later_c)], every)
            rest_ref[p, :, cut(c)] = rest
            if c == 0:
                sum_ref[p] = rest[:, :LANES] + soft_ref[p, :, :LANES].astype(f32)

    def weigh(p):
        for c in range(tiles):
            weight = jnp.exp2(gap_ref[p, :, cut(c)] - rest_ref[p, :, cut(c)])
            weight_ref[p, :, cut(c)] = weight.astype(bf16)
        all_ref[p] = jnp.broadcast_to(sum_ref[p, :, :1], (mine, LANES))

    def gather(b, source, p, valid, fresh):
        portion = mm(weight_ref[p], got_ref[source, :rows])
        total = all_ref[p]
        if fresh:
            acc = portion
            run = total
        else:
            run = run_ref[b]
            acc = acc_ref[b] + portion * jnp.exp2(-run)
            run = run + total
        acc_ref[b] = jnp.where(valid, acc, acc_ref[b])
        run_ref[b] = jnp.where(valid, run, run_ref[b])

    def diagonal(k, _):
        for p in range(2):
            i = 2 * k + p
            old = jnp.minimum(jnp.maximum(i - 3, 0), blocks - 1)
            now = jnp.minimum(i, blocks - 1)
            gather(old, old, 1 - p, (i >= 3) & (i < blocks + 3), True)
            weigh(p)
            total_up(1 - p)
            soften(now, now, p, True)
        return 0

    lax.fori_loop(0, (blocks + 4) // 2, diagonal, 0)
    count = blocks * (blocks - 1) // 2

    def step(k, state):
        for p in range(2):
            i = 2 * k + p
            gather(*state[0:2], 1 - p, (i >= 3) & (i < count + 3), False)
            weigh(p)
            total_up(1 - p)
            b, source = state[6:8]
            soften(b, source, p, False)
            wrap = source == 0
            more = i + 1 < count
            b_next = jnp.where(more, jnp.where(wrap, b + 1, b), b)
            next_source = jnp.where(more, jnp.where(wrap, b, source - 1), source)
            state = (*state[2:], b_next, next_source)
        return state

    if count > 0:
        lax.fori_loop(0, (count + 4) // 2, step, (jnp.int32(1), jnp.int32(0)) * 4)

    few = sub // 2
    keep = lax.broadcasted_iota(jnp.int32, (few, LANES), 1) < HEAD_DIM

    def finish(b, out_at):
        acc = acc_ref[b]
        turned = pltpu.roll(acc, HEAD_DIM, 1)
        for t in range(parts):
            left = turned[t * sub : t * sub + few]
            right = acc[t * sub + few : (t + 1) * sub]
            out_at[t] = jnp.where(keep, left, right).astype(bf16)

    if len(out_refs) > 1:
        for k, ref in enumerate(out_refs):
            for side in range(TOPK):
                finish(lax.axis_index("ep") ^ (k * TOPK + side), ref.at[side])
    else:

        def each(b, _):
            finish(b, out_refs[0].at[b])
            return 0

        lax.fori_loop(0, blocks, each, 0)


def project_with(source, weights, out_ref, *, few, heads, sharers):
    low = lax.broadcasted_iota(jnp.int32, (few, LANES), 1) < HEAD_DIM
    total = None
    for m, w_ref in enumerate(weights):
        strips = []
        for s in range(sharers):
            firsts, seconds = [], []
            for h in range(0, heads, 2):
                a = source(m, h * sharers + s).astype(f32)
                b = source(m, (h + 1) * sharers + s).astype(f32)
                firsts.append(jnp.where(low, a, pltpu.roll(b, HEAD_DIM, 1)))
                seconds.append(jnp.where(low, pltpu.roll(a, HEAD_DIM, 1), b))
            strips.append(jnp.concatenate(firsts, axis=1))
            strips.append(jnp.concatenate(seconds, axis=1))
        left = jnp.concatenate(strips, axis=0).astype(bf16)
        part = mm(left, w_ref[...])
        total = part if total is None else total + part
    out_ref[...] = total.astype(bf16)


def project_body(got_ref, *refs, heads, sharers, parts):
    here = lax.axis_index("tp")
    project_with(
        lambda m, ep: got_ref[ep * parts + (here ^ m)],
        refs[:-1],
        refs[-1],
        few=got_ref.shape[1],
        heads=heads,
        sharers=sharers,
    )


def sides_body(*refs):
    sources, (kept, given) = refs[:GROUPS], refs[GROUPS:]
    for k, source in enumerate(sources):
        kept[k] = source[0]
        given[k] = source[1]


def parts_body(kept, given, *outs):
    here = lax.axis_index("tp")
    for m, out in enumerate(outs):
        for k in range(GROUPS):
            for side, source in enumerate((kept, given)):
                out[k * TOPK + side] = source[k, here ^ m]


def project_pair_body(*refs, heads):
    here = lax.axis_index("ep")
    sources = refs[:4]
    project_with(
        lambda m, ep: sources[m][here ^ ep],
        refs[4:8],
        refs[8],
        few=sources[0].shape[1],
        heads=heads,
        sharers=TOPK,
    )


def stage_body(*refs):
    half = len(refs) // 2
    for a, b in zip(refs[:half], refs[half:]):
        b[...] = a[...]


def spread(piece, size):
    cross = [(i, i ^ 2) for i in range(size)]
    beside = [(i, i ^ 1) for i in range(size)]
    far = lax.ppermute(piece, "tp", cross)
    near = lax.ppermute(piece, "tp", beside)
    return (piece, near, far, lax.ppermute(far, "tp", beside))


def mixer(query_rows, key_rows, value_rows, key_bias, out_pieces, paired):
    rows = query_rows.shape[0]
    heads = query_rows.shape[1] // HEAD_DIM
    ep_count = lax.axis_size("ep")
    parts = lax.axis_size("tp")
    sharers = ep_count // heads
    sub = rows // parts // sharers
    mine = sub * parts
    tall = rows + mine // 2
    bias_type = jax.ShapeDtypeStruct((key_bias.shape[0] // KEY_TILE, KEY_TILE), f32)
    attend_type = jax.ShapeDtypeStruct((ep_count, parts, sub // 2, LANES), bf16)
    work = 3 * ep_count * ep_count * mine * rows * LANES
    scratch = [
        pltpu.VMEM((ep_count, mine, LANES), f32),
        pltpu.VMEM((ep_count, mine, LANES), f32),
        pltpu.VMEM((2, mine, rows), f32),
        pltpu.VMEM((2, mine, rows), f32),
        pltpu.VMEM((2, mine, rows), bf16),
        pltpu.VMEM((2, mine, rows), bf16),
        pltpu.VMEM((2, mine, LANES), f32),
        pltpu.VMEM((2, mine, LANES), f32),
    ]
    sizes = {"rows": rows, "sub": sub, "parts": parts}
    if paired:
        bias, *packed = call(
            functools.partial(pack_pair_body, heads=heads, parts=parts),
            [bias_type] + [jax.ShapeDtypeStruct((tall + mine // 2, LANES), bf16)] * GROUPS,
            [whole(key_bias.T)] + [whole(query_rows)] * 3,
            12,
            scratch=[pltpu.VMEM((heads, tall + mine // 2, LANES), bf16)],
        )(key_bias.T, query_rows, key_rows, value_rows)
        own = [packed[0]]
        for k in range(1, GROUPS):
            pairs = [(i, i ^ (k * TOPK)) for i in range(ep_count)]
            own.append(lax.ppermute(packed[k], "ep", pairs))
        across = [(i, i ^ 1) for i in range(ep_count)]
        theirs = [lax.ppermute(piece, "ep", across) for piece in own]
        block = (parts, sub // 2, LANES)
        attended = call(
            functools.partial(attend_pair_body, **sizes),
            [jax.ShapeDtypeStruct((TOPK, *block), bf16)] * GROUPS,
            [VMEM] * (1 + 2 * GROUPS),
            16,
            flops=work,
            scratch=[pltpu.VMEM((ep_count, tall, LANES), bf16)] + scratch,
        )(bias, *own, *theirs)
        attended = list(attended)
        for k in range(1, GROUPS):
            pairs = [(i, i ^ (k * TOPK)) for i in range(ep_count)]
            attended[k] = lax.ppermute(attended[k], "ep", pairs)
        side_type = jax.ShapeDtypeStruct((GROUPS, *block), bf16)
        kept, given = call(sides_body, [side_type] * 2, [VMEM] * GROUPS, 4)(*attended)
        given = lax.ppermute(given, "ep", across)
        by_part = call(
            parts_body,
            [jax.ShapeDtypeStruct((ep_count, sub // 2, LANES), bf16)] * parts,
            [VMEM] * 2,
            4,
        )(kept, given)
        by_part = list(by_part)
        for m in range(1, parts):
            pairs = [(i, i ^ m) for i in range(parts)]
            by_part[m] = lax.ppermute(by_part[m], "tp", pairs)
        return call(
            functools.partial(project_pair_body, heads=heads),
            jax.ShapeDtypeStruct((rows // parts, out_pieces[0].shape[1]), bf16),
            [VMEM] * 8,
            12,
            flops=2 * rows * heads * HEAD_DIM * out_pieces[0].shape[1],
        )(*by_part, *out_pieces)
    else:
        bias, outgoing = call(
            functools.partial(pack_body, heads=heads, sharers=sharers, parts=parts),
            [bias_type, jax.ShapeDtypeStruct((ep_count, tall, LANES), bf16)],
            [whole(key_bias.T)] + [whole(query_rows)] * 3,
            12,
        )(key_bias.T, query_rows, key_rows, value_rows)
        got = exchange(outgoing, "ep")
        attended = call(
            functools.partial(attend_body, **sizes),
            attend_type,
            [VMEM, VMEM],
            16,
            flops=work,
            scratch=scratch,
        )(got, bias)
    attended = attended.reshape(ep_count * parts, sub // 2, LANES)
    back = exchange(attended, ("ep", "tp"))
    return call(
        functools.partial(project_body, heads=heads, sharers=sharers, parts=parts),
        jax.ShapeDtypeStruct((rows // parts, out_pieces[0].shape[1]), bf16),
        [VMEM] * 5,
        12,
        flops=2 * rows * heads * HEAD_DIM * out_pieces[0].shape[1],
    )(back, *out_pieces)


def route_body(x_ref, gain_ref, pick_ref, weight_ref, *outs, cap):
    out_refs, turn_ref = outs[:GROUPS], outs[GROUPS]
    tokens, width = x_ref.shape
    z = spot_of(TOPK)[2]
    pick = pick_ref[...]
    lanes = GROUPS * 2
    group = lax.broadcasted_iota(jnp.int32, (lanes, tokens), 0)
    inside = (pick[0:1] >= group * TOPK) & (pick[0:1] < (group + 1) * TOPK)
    match = jnp.where(inside, 1.0, 0.0)
    before = (
        lax.broadcasted_iota(jnp.int32, (tokens, tokens), 0)
        < lax.broadcasted_iota(jnp.int32, (tokens, tokens), 1)
    )
    rank = mm(match.astype(bf16), jnp.where(before, 1.0, 0.0).astype(bf16))
    first = ((group ^ z) * cap).astype(f32)
    slot = jnp.sum(match * (rank + first), axis=0, keepdims=True).astype(jnp.int32)
    place = lax.broadcasted_iota(jnp.int32, (GROUPS * cap, tokens), 0) == slot
    place = jnp.where(place, 1.0, 0.0)
    weight = weight_ref[...]
    odd = (pick & 1) == 1
    one = jnp.sum(jnp.where(odd, weight, 0.0), axis=0, keepdims=True)
    zero = jnp.sum(jnp.where(odd, 0.0, weight), axis=0, keepdims=True)
    line = lax.broadcasted_iota(jnp.int32, (LANES, tokens), 0)
    value = jnp.where((line & 1) == 1, one, zero)
    high = value.astype(bf16).astype(f32)
    extra = jnp.where(line < 2, high, value - high).astype(bf16)
    place_b = place.astype(bf16)
    turn_ref[...] = place.T.astype(bf16)
    wide = x_ref[...].astype(f32)
    normed = (
        wide
        * lax.rsqrt(jnp.mean(wide * wide, axis=1, keepdims=True) + norm_eps)
        * gain_ref[...]
    ).astype(bf16)
    for k, ref in enumerate(out_refs):
        strip = place_b[k * cap : (k + 1) * cap]
        ref[:, :width] = mm(strip, normed).astype(bf16)
        ref[:, width:] = lax.dot_general(
            strip, extra, (((1,), (1,)), ((), ())), preferred_element_type=f32
        ).astype(bf16)


def expand_body(*refs):
    rows, gates, ups = refs[:GROUPS], refs[GROUPS : GROUPS + 4], refs[GROUPS + 4 : GROUPS + 8]
    out_ref, mix_ref = refs[GROUPS + 8 :]
    width, part = gates[0].shape
    x = jnp.concatenate([r[:, :width] for r in rows], axis=0)
    mix_ref[...] = jnp.concatenate([r[:, width:] for r in rows], axis=0)
    for i in range(4):
        gate = mm(x, gates[i][...])
        up = mm(x, ups[i][...])
        out_ref[:, i * part : (i + 1) * part] = (gate / (1.0 + jnp.exp(-gate)) * up).astype(bf16)


def contract_body(h_ref, d0, d1, d2, d3, *out_refs, starts):
    part = d0.shape[0]
    total = None
    for i, d in enumerate((d0, d1, d2, d3)):
        got = mm(h_ref[:, i * part : (i + 1) * part], d[...])
        total = got if total is None else total + got
    for start, ref in zip(starts, out_refs):
        ref[...] = total[start : start + ref.shape[0]].astype(bf16)


def join_body(own_ref, other_ref, mix_ref, out_ref, *, first):
    extra = mix_ref[first : first + own_ref.shape[0]].astype(f32)
    zero = extra[:, 0:1] + extra[:, 2:3]
    one = extra[:, 1:2] + extra[:, 3:4]
    odd = spot_of(TOPK)[0] == 1
    mine = jnp.where(odd, one, zero)
    theirs = jnp.where(odd, zero, one)
    out_ref[...] = (own_ref[...].astype(f32) * mine + other_ref[...].astype(f32) * theirs).astype(bf16)


def restore_body(turn_ref, *refs):
    out_ref = refs[-1]
    rows = jnp.concatenate([ref[...] for ref in refs[:-1]], axis=0)
    total = mm(turn_ref[...], rows)
    out_ref[...] = total.astype(bf16)


def paired_experts(moe_input, moe_gain, expert_pick, route_weight, gates, ups, downs):
    tokens, width = moe_input.shape
    ep_count = lax.axis_size("ep")
    cap = GROUPS * tokens // ep_count

    def along(k):
        return [(i, i ^ (k * TOPK)) for i in range(ep_count)]

    across = [(i, i ^ 1) for i in range(ep_count)]
    row_type = jax.ShapeDtypeStruct((cap, width + LANES), bf16)
    route_args = (moe_input, moe_gain.reshape(1, width), expert_pick.T, route_weight.T)
    *sent, turn = call(
        functools.partial(route_body, cap=cap),
        [row_type] * GROUPS + [jax.ShapeDtypeStruct((tokens, GROUPS * cap), bf16)],
        [whole(a) for a in route_args],
        12,
    )(*route_args)
    own = [sent[0]] + [lax.ppermute(sent[k], "ep", along(k)) for k in range(1, GROUPS)]
    theirs = [lax.ppermute(rows, "ep", across) for rows in own]
    part = gates[0].shape[2]
    count = GROUPS * cap
    gates = [g[0] for g in gates]
    ups = [u[0] for u in ups]
    piece_type = jax.ShapeDtypeStruct(gates[0].shape, bf16)
    gates[0], ups[0] = call(stage_body, [piece_type] * 2, [VMEM] * 2, 8)(gates[0], ups[0])
    half = cap // 2
    pieces = [(0, 0, cap), (1, 0, cap), (2, 0, half), (3, 0, cap), (2, half, half)]
    starts = [k * cap + first for k, first, _ in pieces]
    results = {}
    for side, arrived in (("a", own), ("b", theirs)):
        hidden, got = call(
            expand_body,
            [
                jax.ShapeDtypeStruct((count, 4 * part), bf16),
                jax.ShapeDtypeStruct((count, LANES), bf16),
            ],
            [VMEM] * (GROUPS + 8),
            16,
            flops=4 * count * width * 4 * part,
        )(*arrived, *gates, *ups)
        if side == "a":
            mix = got
        results[side] = call(
            functools.partial(contract_body, starts=starts),
            [jax.ShapeDtypeStruct((rows, width), bf16) for _, _, rows in pieces],
            [VMEM] * 5,
            16,
            flops=2 * count * width * 4 * part,
        )(hidden, *[d[0] for d in downs])
    others, returned = {}, {}
    for i in RETURN_ORDER:
        others[i] = lax.ppermute(results["b"][i], "ep", across)
    for i in RETURN_ORDER:
        k, _, rows = pieces[i]
        joined = call(
            functools.partial(join_body, first=starts[i]),
            jax.ShapeDtypeStruct((rows, width), bf16),
            [VMEM] * 3,
            4,
        )(results["a"][i], others[i], mix)
        returned[i] = lax.ppermute(joined, "ep", along(k)) if k else joined
    order = sorted(range(len(pieces)), key=lambda i: starts[i])
    return call(
        restore_body, jax.ShapeDtypeStruct((tokens, width), bf16), [VMEM] * (len(pieces) + 1), 8
    )(turn, *[returned[i] for i in order])


def expand(arrived, gate_weights, up_weights):
    gate_in = jnp.einsum("necm,emf->necf", arrived, gate_weights, preferred_element_type=f32)
    up_in = jnp.einsum("necm,emf->necf", arrived, up_weights, preferred_element_type=f32)
    return (jax.nn.silu(gate_in) * up_in).astype(bf16)


def contract(hidden, down_weights):
    return jnp.einsum("necf,efm->necm", hidden, down_weights, preferred_element_type=f32)


def any_experts(moe_input, moe_gain, expert_pick, route_weight, w_gate, w_up, w_down):
    ep_count = lax.axis_size("ep")
    token_count = moe_input.shape[0]
    widened = moe_input.astype(f32)
    normed = (
        widened
        * lax.rsqrt(jnp.mean(widened * widened, axis=1, keepdims=True) + norm_eps)
        * moe_gain
    ).astype(bf16)
    local_experts = w_gate.shape[0]
    expert_total = local_experts * ep_count
    capacity = GROUPS * token_count // expert_total
    picks = expert_pick.reshape(-1)
    matches = (picks[:, None] == jnp.arange(expert_total, dtype=jnp.int32)[None, :]).astype(
        jnp.int32
    )
    ranks = jnp.sum((jnp.cumsum(matches, axis=0) - matches) * matches, axis=1)
    slots = picks * capacity + ranks
    owners = jnp.arange(picks.shape[0], dtype=jnp.int32) // TOPK
    table = jnp.full((expert_total * capacity,), token_count, jnp.int32).at[slots].set(owners)
    padded = jnp.concatenate([normed, jnp.zeros((1, normed.shape[1]), bf16)], axis=0)
    outgoing = padded[table].reshape(ep_count, local_experts, capacity, normed.shape[1])
    arrived = lax.all_to_all(outgoing, "ep", split_axis=0, concat_axis=0, tiled=True)
    gate_all, up_all, down_all = (
        lax.all_gather(w_gate, "tp", axis=2, tiled=True),
        lax.all_gather(w_up, "tp", axis=2, tiled=True),
        lax.all_gather(w_down, "tp", axis=1, tiled=True),
    )
    served = contract(expand(arrived, gate_all, up_all), down_all).astype(bf16)
    returned = lax.all_to_all(served, "ep", split_axis=0, concat_axis=0, tiled=True)
    flat = returned.reshape(expert_total * capacity, returned.shape[3])
    chosen = flat[slots].reshape(token_count, TOPK, flat.shape[1]).astype(f32)
    return jnp.sum(chosen * route_weight[:, :, None], axis=1).astype(bf16)


def local(
    query_rows,
    key_rows,
    value_rows,
    key_bias,
    out_weight,
    moe_input,
    moe_gain,
    expert_pick,
    route_weight,
    w_gate,
    w_up,
    w_down,
):
    tp_size = lax.axis_size("tp")
    paired = is_paired(lax.axis_size("ep"), w_gate.shape[0])
    paired = paired and query_rows.shape[1] == GROUPS * HEAD_DIM
    if paired:
        gates = spread(w_gate, tp_size)
        ups = spread(w_up, tp_size)
        downs = spread(w_down, tp_size)
        routed_out = paired_experts(
            moe_input, moe_gain, expert_pick, route_weight, gates, ups, downs
        )
    else:
        routed_out = any_experts(
            moe_input, moe_gain, expert_pick, route_weight, w_gate, w_up, w_down
        )
    out_pieces = spread(out_weight, tp_size)
    mixer_out = mixer(query_rows, key_rows, value_rows, key_bias, out_pieces, paired)
    return (mixer_out, routed_out)


def is_paired(ep_count, local_experts):
    return local_experts == 1 and ep_count == GROUPS * TOPK


def solution(mesh):
    placed = (
        P("ep", "tp"),
        P("ep", "tp"),
        P("ep", "tp"),
        P(None, "tp"),
        P("tp", None),
        P(("ep", "tp"), None),
        P(),
        P(("ep", "tp"), None),
        P(("ep", "tp"), None),
        P("ep", None, "tp"),
        P("ep", None, "tp"),
        P("ep", "tp", None),
    )
    return jax.shard_map(
        local,
        mesh=mesh,
        in_specs=placed,
        out_specs=(P(("ep", "tp"), None), P(("ep", "tp"), None)),
        check_vma=False,
    )
```
